256 devices in a mesh: fs: 32 (over z, x), tp: 8 (over y, core).
Axes of the slice: x: 4, y: 4, z: 8, core: 2. Of those that a mesh axis runs over, the one named last changes fastest.
Arguments:
- tokens: bfloat16 [6144, 2048], P('fs'), may hold values from -6 to 6
- norm_gain: float32 [2048], P('fs'), may hold values from 0.1 to 1.9
- expert_gate: float32 [64, 2048, 1024], P(None, 'fs', 'tp'), may hold values from -0.125 to 0.125
- expert_up: float32 [64, 2048, 1024], P(None, 'fs', 'tp'), may hold values from -0.125 to 0.125
- expert_down: float32 [64, 1024, 2048], P(None, 'fs', 'tp'), may hold values from -0.1875 to 0.1875
- shared_gate: float32 [2048, 1024], P('fs', 'tp'), may hold values from -0.125 to 0.125
- shared_up: float32 [2048, 1024], P('fs', 'tp'), may hold values from -0.125 to 0.125
- shared_down: float32 [1024, 2048], P('fs', 'tp'), may hold values from -0.1875 to 0.1875
- expert_ids: int32 [6144, 8], P('fs'), may hold values from 0 to 63, all different within a row; in each aligned block of 192 rows (0 to 191, 192 to 383, ...) at most 48 rows name the same one
- route_weights: float32 [6144, 8], P('fs'), may hold values from 0.25 to 1
Outputs:
- gate_ready: bfloat16 [64, 2048, 1024], P('fs', None, 'tp')
- up_ready: bfloat16 [64, 2048, 1024], P('fs', None, 'tp')
- down_ready: bfloat16 [64, 1024, 2048], P('fs', None, 'tp')
- shared_gate_ready: bfloat16 [2048, 1024], P(None, 'tp')
- shared_up_ready: bfloat16 [2048, 1024], P(None, 'tp')
- shared_down_ready: bfloat16 [1024, 2048], P(None, 'tp')
- mixed: bfloat16 [6144, 2048], P('fs', 'tp')
The draws below stay inside these ranges and needn't reach their ends.
Inputs may be any that keep to these rules, and one draw needn't show every extreme that they name: `expert_ids`: each row names 8 different experts. Among the 192 rows of one index of fs no expert is named more than 48 times, and in every draw some expert is named exactly 48 times there.
All inputs are finite; a program needn't handle non-finite values.
Results may differ from the reference program's by a relative error of at most 0.0085.
Values may be sent and summed in bfloat16 or wider, within the bound.
A program may use at most 128 MiB of HBM per device.

```python
import math
import jax
import jax.numpy as jnp
import numpy as np
from jax import lax

D = 2048
DE = 1024
TOP_K = 8
TOK_DEV = 192
EXPERTS = 64
TOKENS = 6144
CAPE = 48
N_FS = 32


def steps_of(own_key, extent, pieces, low, top_value):
    level, own = 1.0, jax.random.fold_in(own_key, 6)
    for axis_at, parts in pieces:
        draws = jnp.exp(jax.random.uniform(jax.random.fold_in(own, axis_at), (parts,), jnp.float32, low / len(pieces), top_value / len(pieces)))
        level = level * jnp.repeat(draws, extent[axis_at] // parts).reshape([-1 if axis == axis_at else 1 for axis in range(len(extent))])
    return level


def routed_block(key, own, number, rows, count, top, limit, slope):
    ranking = jax.random.permutation(key, count)
    crowded, common = shares(count, rows * top, limit, slope, True), shares(count, rows * top, limit, slope, False)
    places = jnp.arange(count)

    def named(tallies, offset_by):
        used = int((tallies > 0).sum())
        fixed = max(1, used // 4)
        moved = fixed + (places - fixed + offset_by * (used - fixed)) % max(1, count - fixed)
        return jnp.zeros((count,), jnp.int32).at[ranking[jnp.where(places < fixed, places, moved)]].set(jnp.asarray(tallies, jnp.int32))

    tallies = jnp.where(number % 4 == 0, named(crowded, number // 4), named(common, number - number // 4 - 1))
    mixed = jax.random.permutation(jax.random.fold_in(own, 3), count)
    giver, receiver = mixed[0:count // 2 * 2:2], mixed[1:count // 2 * 2:2]
    slack = jnp.minimum(tallies[giver] - 1, limit - tallies[receiver]) // 2
    slack = jnp.where((giver == ranking[0]) | (receiver == ranking[0]) | (tallies[receiver] == 0), 0, jnp.maximum(slack, 0))
    moved = jax.random.randint(jax.random.fold_in(own, 4), (count // 2,), 0, 1 << 20) % (slack + 1)
    tallies = tallies.at[giver].add(-moved).at[receiver].add(moved)
    members = jnp.searchsorted(jnp.cumsum(tallies), jnp.arange(rows * top), side="right").astype(jnp.int32)
    grid = members.reshape(top, rows).T
    grid = grid[jax.random.permutation(jax.random.fold_in(own, 1), rows)]
    offset_by = jax.random.randint(jax.random.fold_in(own, 2), (rows, 1), 0, top)
    return jnp.take_along_axis(grid, (jnp.arange(top)[None, :] + offset_by) % top, axis=1)


def shares(count, total, bound, lean, full):
    portions = [(1 << 20) // math.isqrt(rank ** lean) + 1 for rank in range(1, count + 1)]
    largest = bound if full else min(bound, max(-(-total // count), total * portions[0] // sum(portions)))
    least = 1 if total - largest >= count - 1 else 0
    counts, spare = [largest] + [least] * (count - 1), total - largest - least * (count - 1)
    while spare > 0:
        candidates = [i for i in range(1, count) if counts[i] < largest] or [i for i in range(1, count) if counts[i] < bound]
        pool, remaining = sum([portions[i] for i in candidates]), spare
        for i in candidates:
            more = min(bound - counts[i], max(1, remaining * portions[i] // pool), spare)
            counts[i] = counts[i] + more
            spare = spare - more
    return np.array(counts)


def scatter_about(own_key, dims, spread, reach, cuts=(), kind=jnp.bfloat16):
    values = spread * jax.random.normal(own_key, dims, jnp.float32)
    if cuts:
        values = values * steps_of(own_key, dims, cuts, -0.22, 0.18)
    return jnp.clip(values, -reach, reach).astype(kind)


def setup_inputs(seed: int = 0) -> dict:
    arg_keys = jax.random.split(jax.random.key(seed), 11)
    tokens = scatter_about(arg_keys[0], (TOKENS, D), 1.0, 6.0, ((0, 32),))
    norm_gain = jnp.clip(1.0 + 0.18 * jax.random.normal(arg_keys[1], (D,), jnp.float32), 0.1, 1.9)
    expert_gate = scatter_about(arg_keys[2], (EXPERTS, D, DE), D ** -0.5, 0.125, ((1, 32), (2, 8)), jnp.float32)
    expert_up = scatter_about(arg_keys[3], (EXPERTS, D, DE), D ** -0.5, 0.125, ((1, 32), (2, 8)), jnp.float32)
    expert_down = scatter_about(arg_keys[4], (EXPERTS, DE, D), DE ** -0.5, 0.1875, ((1, 32), (2, 8)), jnp.float32)
    shared_gate = scatter_about(arg_keys[5], (D, DE), D ** -0.5, 0.125, ((0, 32), (1, 8)), jnp.float32)
    shared_up = scatter_about(arg_keys[6], (D, DE), D ** -0.5, 0.125, ((0, 32), (1, 8)), jnp.float32)
    shared_down = scatter_about(arg_keys[7], (DE, D), DE ** -0.5, 0.1875, ((0, 32), (1, 8)), jnp.float32)
    expert_ids_keys = jax.random.split(jax.random.fold_in(arg_keys[8], 1), TOKENS // TOK_DEV)
    expert_ids_turns = jax.random.permutation(jax.random.fold_in(arg_keys[8], 3), TOKENS // TOK_DEV)
    expert_ids = jax.vmap(lambda own, number: routed_block(jax.random.fold_in(arg_keys[8], 2), own, number, TOK_DEV, EXPERTS, TOP_K, CAPE, 1))(expert_ids_keys, expert_ids_turns).reshape((TOKENS, TOP_K))
    route_weights = jnp.clip(jnp.exp(math.log(1.0) - 1.3862944 * jax.random.uniform(arg_keys[9], (TOKENS, TOP_K), jnp.float32) ** steps_of(arg_keys[9], (TOKENS, TOP_K), ((0, 32),), -0.2, 0.2)), 0.25, 1.0)
    return {"tokens": tokens, "norm_gain": norm_gain, "expert_gate": expert_gate, "expert_up": expert_up, "expert_down": expert_down, "shared_gate": shared_gate, "shared_up": shared_up, "shared_down": shared_down, "expert_ids": expert_ids, "route_weights": route_weights}


EPS = 1e-06

def reference(tokens, norm_gain, expert_gate, expert_up, expert_down, shared_gate, shared_up, shared_down, expert_ids, route_weights):
    gain = norm_gain.astype(jnp.float32)
    gate_ready = (expert_gate * gain[None, :, None]).astype(jnp.bfloat16)
    up_ready = (expert_up * gain[None, :, None]).astype(jnp.bfloat16)
    down_ready = expert_down.astype(jnp.bfloat16)
    shared_gate_ready = (shared_gate * gain[:, None]).astype(jnp.bfloat16)
    shared_up_ready = (shared_up * gain[:, None]).astype(jnp.bfloat16)
    shared_down_ready = shared_down.astype(jnp.bfloat16)
    wide = tokens.astype(jnp.float32)
    normed = (wide * lax.rsqrt(lax.optimization_barrier(jnp.mean(wide * wide, axis=-1, keepdims=True)) + EPS)).astype(jnp.bfloat16)
    shared_first = jnp.dot(normed, shared_gate_ready, preferred_element_type=jnp.float32)
    shared_second = jnp.dot(normed, shared_up_ready, preferred_element_type=jnp.float32)
    shared_hidden = (jax.nn.silu(shared_first) * shared_second).astype(jnp.bfloat16)
    shared_out = jnp.dot(shared_hidden, shared_down_ready, preferred_element_type=jnp.float32)
    experts = expert_gate.shape[0]
    tok_block = tokens.shape[0] // N_FS
    capacity = 2 * tok_block * TOP_K // experts
    chosen = expert_ids.reshape(N_FS, tok_block * TOP_K).astype(jnp.int32)
    onehot = (chosen[..., None] == jnp.arange(experts, dtype=jnp.int32)).astype(jnp.int32)
    ranks = (lax.optimization_barrier(jnp.sum(jnp.cumsum(onehot, axis=1) * onehot, axis=-1)) - 1).astype(jnp.int32)
    blocks = jnp.broadcast_to(jnp.arange(N_FS, dtype=jnp.int32)[:, None], chosen.shape)
    owners = (blocks * tok_block + jnp.arange(tok_block * TOP_K, dtype=jnp.int32)[None, :] // TOP_K).astype(jnp.int32)
    slot_token = jnp.zeros((experts, N_FS, capacity), jnp.int32).at[chosen, blocks, ranks].set(owners)
    slot_weight = jnp.zeros((experts, N_FS, capacity), jnp.float32).at[chosen, blocks, ranks].set(route_weights.reshape(N_FS, -1).astype(jnp.float32))

    def one_expert(total, index):
        which = slot_token[index].reshape(-1)
        rows = normed[which]
        first = jnp.dot(rows, gate_ready[index], preferred_element_type=jnp.float32)
        second = jnp.dot(rows, up_ready[index], preferred_element_type=jnp.float32)
        hidden = (jax.nn.silu(first) * second).astype(jnp.bfloat16)
        result = jnp.dot(hidden, down_ready[index], preferred_element_type=jnp.float32).astype(jnp.bfloat16)
        result = lax.optimization_barrier(result).astype(jnp.float32)
        return (total.at[which].add(result * slot_weight[index].reshape(-1)[:, None]), None)
    routed, _ = lax.scan(one_expert, jnp.zeros(tokens.shape, jnp.float32), jnp.arange(experts, dtype=jnp.int32))
    mixed = (shared_out + routed).astype(jnp.bfloat16)
    return (gate_ready, up_ready, down_ready, shared_gate_ready, shared_up_ready, shared_down_ready, mixed)
```

```python
import jax
import jax.numpy as jnp
from jax import lax
from jax.experimental import pallas as pl
from jax.experimental.pallas import tpu as pltpu
from jax.sharding import PartitionSpec as P

EPS = 1e-06
NZ, NX, NY = 8, 4, 4
NF, NT = NZ * NX, NY * 2
D, DE, TOK, TOP_K, EXPERTS = 2048, 1024, 192, 8, 64
CAP = 2 * TOK * TOP_K // EXPERTS
PER = EXPERTS // NF
DC = D // NT
HC = DE // NT
KR, KD = D // NF, DE // NF
ROWS = TOK + KR + KD + 16
CUT = 160
SRC = NX * CAP
OFFS = (0, -1, 1, -2, 2, -3, 3, 4)
BF, F32 = jnp.bfloat16, jnp.float32
MESH = pl.DeviceIdType.MESH


def silu_mul(a, b):
    return (a * (1.0 / (1.0 + jnp.exp(-a)))) * b


def kernel(
    tblk, nfull, wgu, wdn,
    gu_o, dn_o, sw_o, ret_o, sh_o,
    ta, xg, gu, dn, hg, hs, og, ret, shv,
    zr, xr, br, bs, cr, cs, er, dr, ss, lo,
):
    fs, tp = lax.axis_index("fs"), lax.axis_index("tp")
    z, x = fs // NX, lax.rem(fs, NX)
    y, c = tp // 2, lax.rem(tp, 2)

    def fsn(dz, dx):
        return lax.rem(z + dz + NZ, NZ) * NX + lax.rem(x + dx + NX, NX)

    def tpn(dy, dc):
        return lax.rem(y + dy + NY, NY) * 2 + lax.rem(c + dc, 2)

    yp, ym, sib = tpn(1, 0), tpn(-1, 0), tpn(0, 1)

    def copy(src, dst, s, r, f, t):
        return pltpu.make_async_remote_copy(
            src_ref=src, dst_ref=dst, send_sem=s, recv_sem=r, device_id=(f, t), device_id_type=MESH
        )

    def arrived(dst, r):
        copy(dst, dst, ss.at[0], r, fs, sib).wait_recv()

    barrier = pltpu.get_barrier_semaphore()
    for k in range(1, NF):
        pl.semaphore_signal(barrier, inc=1, device_id=(lax.rem(fs + k, NF), tp), device_id_type=MESH)
    for t in (yp, ym, sib):
        pl.semaphore_signal(barrier, inc=1, device_id=(fs, t), device_id_type=MESH)
    pl.semaphore_wait(barrier, NF - 1 + 3)

    zp, zm, xp, xm = fsn(1, 0), fsn(-1, 0), fsn(0, 1), fsn(0, -1)

    def zi(i):
        return lax.rem(z + OFFS[i] + NZ, NZ)

    def z_step(i):
        s = zi(i) * NX + x
        blk = ta.at[s]
        if i == 0:
            copy(tblk, blk, ss.at[0], zr.at[1], zp, tp).start()
            copy(tblk, blk, ss.at[0], zr.at[2], zm, tp).start()
            copy(tblk, blk, ss.at[0], xr.at[0, 0], xp, tp).start()
            copy(tblk, blk, ss.at[0], xr.at[0, 1], xm, tp).start()
            ta[fs] = tblk[...]
            return
        low, high = ta.at[s, pl.ds(0, CUT)], ta.at[s, pl.ds(CUT, ROWS - CUT)]
        if i == 7:
            arrived(low, zr.at[7])
            arrived(high, zr.at[8])
        else:
            arrived(blk, zr.at[i])
            if i == 5:
                copy(low, low, ss.at[0], zr.at[7], zp, tp).start()
            elif i == 6:
                copy(high, high, ss.at[0], zr.at[8], zm, tp).start()
            else:
                copy(blk, blk, ss.at[0], zr.at[i + 2], zp if OFFS[i] < 0 else zm, tp).start()
        copy(blk, blk, ss.at[0], xr.at[i, 0], xp, tp).start()
        copy(blk, blk, ss.at[0], xr.at[i, 1], xm, tp).start()

    def x_step(i):
        left = zi(i) * NX + lax.rem(x + NX - 1, NX)
        right = zi(i) * NX + lax.rem(x + 1, NX)
        arrived(ta.at[left], xr.at[i, 0])
        low = ta.at[left, pl.ds(0, CUT)]
        copy(low, low, ss.at[0], xr.at[i, 2], xp, tp).start()
        arrived(ta.at[right], xr.at[i, 1])
        high = ta.at[right, pl.ds(CUT, ROWS - CUT)]
        copy(high, high, ss.at[0], xr.at[i, 3], xm, tp).start()

    cols = pl.ds(pl.multiple_of(tp * DC, DC), DC)
    hcols = pl.ds(pl.multiple_of(tp * HC, HC), HC)

    def select(i):
        far = zi(i) * NX + lax.rem(x + 2, NX)
        arrived(ta.at[far, pl.ds(0, CUT)], xr.at[i, 2])
        arrived(ta.at[far, pl.ds(CUT, ROWS - CUT)], xr.at[i, 3])
        first = (PER * fs).astype(F32)
        rows = []
        for k in range(NX):
            ids = ta[zi(i) * NX + k, pl.ds(ROWS - 16, 16), pl.ds(0, TOK)].astype(F32)
            for e in range(PER):
                rows.append(jnp.sum(jnp.where(ids == first + e, 1.0, 0.0), axis=0, keepdims=True))
        match = jnp.concatenate(rows, axis=0)
        before = (
            lax.broadcasted_iota(jnp.int32, (TOK, TOK), 0) < lax.broadcasted_iota(jnp.int32, (TOK, TOK), 1)
        )
        upper = jnp.where(before, 1.0, 0.0).astype(BF)
        rank = jnp.dot(match.astype(BF), upper, preferred_element_type=F32)
        place = jnp.where(match > 0.5, rank, -1.0)
        slot = lax.broadcasted_iota(jnp.int32, (CAP, TOK), 0).astype(F32)
        for k in range(NX):
            hot = jnp.concatenate(
                [jnp.where(slot == place[PER * k + e : PER * k + e + 1], 1.0, 0.0) for e in range(PER)], axis=0
            ).astype(BF)
            rows = jnp.dot(hot, ta[zi(i) * NX + k, pl.ds(0, TOK), :], preferred_element_type=F32).astype(BF)
            for e in range(PER):
                xg[i, e, pl.ds(CAP * k, CAP), cols] = rows[CAP * e : CAP * (e + 1)]

    def at(buf, i, w, t):
        return buf.at[i, :, :, pl.ds(pl.multiple_of(t * w, w), w)]

    def half(buf, i, w, t, e):
        return buf.at[i, e, :, pl.ds(pl.multiple_of(t * w, w), w)]

    def tp_send(buf, i, w, s, r, b):
        own = at(buf, i, w, tp)
        copy(own, own, s, r.at[0], fs, yp).start()
        copy(own, own, s, r.at[1], fs, ym).start()
        copy(own, own, s, b, fs, sib).start()

    def tp_pass(buf, i, w, s, r, b):
        a = at(buf, i, w, ym)
        arrived(a, r.at[0])
        h = half(buf, i, w, ym, 0)
        copy(h, h, s, r.at[2], fs, yp).start()
        copy(a, a, s, b, fs, sib).start()
        a = at(buf, i, w, yp)
        arrived(a, r.at[1])
        h = half(buf, i, w, yp, 1)
        copy(h, h, s, r.at[3], fs, ym).start()
        copy(a, a, s, b, fs, sib).start()

    def tp_last(buf, i, w, s, r, b):
        far = tpn(2, 0)
        for e in range(2):
            h = half(buf, i, w, far, e)
            arrived(h, r.at[2 + e])
            copy(h, h, s, b, fs, sib).start()

    def tp_done(buf, i, w, b):
        arrived(buf.at[i, :, :, pl.ds(0, 4 * w)], b)

    peers = [(dz, dx) for dx in (0, 1, 3, 2) for dz in (1, -1, 2, -2, 3, -3, 4, 0)]
    peers = [p for p in peers if p != (0, 0)]

    def send_gu(n):
        f = fsn(*peers[n])
        copy(wgu.at[f], gu.at[:, pl.ds(pl.multiple_of(fs * KR, KR), KR), :], ss.at[3], er.at[0], f, tp).start()

    def send_dn(n):
        f = fsn(*peers[n])
        copy(wdn.at[f], dn.at[:, pl.ds(pl.multiple_of(fs * KD, KD), KD), :], ss.at[4], er.at[1], f, tp).start()

    def gate_up(i):
        for e in range(PER):
            both = jnp.dot(xg[i, e], gu[e], preferred_element_type=F32)
            hg[i, e, :, hcols] = silu_mul(both[:, :HC], both[:, HC:]).astype(BF)

    def down(i):
        for e in range(PER):
            out = jnp.dot(hg[i, e], dn[e], preferred_element_type=F32).astype(BF)
            for k in range(NX):
                og[i, k, pl.ds(CAP * e, CAP), :] = out[CAP * k : CAP * (k + 1)]

    def give_back(i):
        for dx in range(NX):
            k = lax.rem(x + dx, NX)
            if i == 0 and dx == 0:
                ret[fs] = og[0, k]
                continue
            copy(og.at[i, k], ret.at[fs], ss.at[5], dr.at[0], zi(i) * NX + k, tp).start()

    sent_gu, sent_dn = 0, 0
    for tick in range(NZ + 4):
        if tick < NZ:
            z_step(tick)
        if 0 <= tick - 1 < NZ:
            x_step(tick - 1)
        if 0 <= tick - 2 < NZ:
            select(tick - 2)
            tp_send(xg, tick - 2, DC, ss.at[1], br.at[tick - 2], bs.at[tick - 2])
        if 0 <= tick - 3 < NZ:
            tp_pass(xg, tick - 3, DC, ss.at[1], br.at[tick - 3], bs.at[tick - 3])
        if 0 <= tick - 4 < NZ:
            tp_last(xg, tick - 4, DC, ss.at[1], br.at[tick - 4], bs.at[tick - 4])
        for _ in range(4):
            if sent_gu < NF - 1:
                send_gu(sent_gu)
                sent_gu += 1
        if tick == 0:
            gu[:, pl.ds(pl.multiple_of(fs * KR, KR), KR), :] = wgu[fs]
            dn[:, pl.ds(pl.multiple_of(fs * KD, KD), KD), :] = wdn[fs]
        if tick >= NZ:
            for _ in range(8):
                if sent_dn < NF - 1:
                    send_dn(sent_dn)
                    sent_dn += 1
        if tick == NZ + 2:
            sgu = ta[:, pl.ds(TOK, KR), :].reshape(D, 2 * HC)
            both = jnp.dot(nfull[...], sgu, preferred_element_type=F32)
            mid = silu_mul(both[:, :HC], both[:, HC:]).astype(BF)
            hs[0, 0, :, hcols] = mid[: TOK // 2]
            hs[0, 1, :, hcols] = mid[TOK // 2 :]

    shared = (hs, 0, HC, ss.at[6], cr.at[NZ], cs.at[NZ])
    tp_send(*shared)
    arrived(gu.at[:, pl.ds(0, D - KR), :], er.at[0])
    gu_copy = pltpu.make_async_copy(gu, gu_o, lo.at[0])
    gu_copy.start()
    for tick in range(NZ + 3):
        if tick < NZ:
            tp_done(xg, tick, DC, bs.at[tick])
            gate_up(tick)
            tp_send(hg, tick, HC, ss.at[2], cr.at[tick], cs.at[tick])
        if tick == 0:
            tp_pass(*shared)
        elif tick == 1:
            tp_last(*shared)
        if 0 <= tick - 1 < NZ:
            tp_pass(hg, tick - 1, HC, ss.at[2], cr.at[tick - 1], cs.at[tick - 1])
        if 0 <= tick - 2 < NZ:
            tp_last(hg, tick - 2, HC, ss.at[2], cr.at[tick - 2], cs.at[tick - 2])
        if 0 <= tick - 3 < NZ:
            if tick == 3:
                arrived(dn.at[:, pl.ds(0, DE - KD), :], er.at[1])
                dn_copy = pltpu.make_async_copy(dn, dn_o, lo.at[1])
                dn_copy.start()
            tp_done(hg, tick - 3, HC, cs.at[tick - 3])
            down(tick - 3)
            give_back(tick - 3)
    sw_copy = pltpu.make_async_copy(ta.at[:, pl.ds(TOK, KR + KD), :], sw_o, lo.at[2])
    sw_copy.start()
    tp_done(hs, 0, HC, cs.at[NZ])
    sdn = ta[:, pl.ds(TOK + KR, KD), :].reshape(DE, DC)
    for e in range(2):
        shv[pl.ds(e * (TOK // 2), TOK // 2), :] = jnp.dot(hs[0, e], sdn, preferred_element_type=F32)
    sh_copy = pltpu.make_async_copy(shv, sh_o, lo.at[3])
    sh_copy.start()
    arrived(ret.at[pl.ds(0, NF - 1)], dr.at[0])
    ret_copy = pltpu.make_async_copy(ret, ret_o, lo.at[4])
    ret_copy.start()

    def sent(ref, s):
        copy(ref, ref, s, dr.at[0], fs, sib).wait_send()

    sent(ta.at[pl.ds(0, NF - 1)], ss.at[0])
    sent(xg.at[pl.ds(0, NZ - 1)], ss.at[1])
    sent(hg.at[pl.ds(0, NZ - 1)], ss.at[2])
    sent(gu.at[:, pl.ds(0, D - KR), :], ss.at[3])
    sent(dn.at[:, pl.ds(0, DE - KD), :], ss.at[4])
    sent(ret.at[pl.ds(0, NF - 1)], ss.at[5])
    sent(hs.at[0, :, :, pl.ds(0, 7 * HC)], ss.at[6])
    gu_copy.wait()
    dn_copy.wait()
    sw_copy.wait()
    sh_copy.wait()
    ret_copy.wait()


def exchange(tblk, nfull, wgu, wdn):
    vmem, anyw = pl.BlockSpec(memory_space=pltpu.VMEM), pl.BlockSpec(memory_space=pl.ANY)
    dma = pltpu.SemaphoreType.DMA
    return pl.pallas_call(
        kernel,
        out_shape=(
            jax.ShapeDtypeStruct((PER, D, 2 * HC), BF),
            jax.ShapeDtypeStruct((PER, DE, DC), BF),
            jax.ShapeDtypeStruct((NF, KR + KD, DC), BF),
            jax.ShapeDtypeStruct((NF, PER * CAP, DC), BF),
            jax.ShapeDtypeStruct((TOK, DC), F32),
        ),
        in_specs=[vmem] * 4,
        out_specs=(anyw,) * 5,
        scratch_shapes=[
            pltpu.VMEM((NF, ROWS, DC), BF),
            pltpu.VMEM((NZ, PER, SRC, D), BF),
            pltpu.VMEM((PER, D, 2 * HC), BF),
            pltpu.VMEM((PER, DE, DC), BF),
            pltpu.VMEM((NZ, PER, SRC, DE), BF),
            pltpu.VMEM((1, 2, TOK // 2, DE), BF),
            pltpu.VMEM((NZ, NX, PER * CAP, DC), BF),
            pltpu.VMEM((NF, PER * CAP, DC), BF),
            pltpu.VMEM((TOK, DC), F32),
            dma((9,)), dma((NZ, 4)), dma((NZ, 4)), dma((NZ,)), dma((NZ + 1, 4)), dma((NZ + 1,)),
            dma((2,)), dma((1,)), dma((7,)), dma((5,)),
        ],
        compiler_params=pltpu.CompilerParams(
            collective_id=0, has_side_effects=True, vmem_limit_bytes=56 * 1024 * 1024
        ),
    )(tblk, nfull, wgu, wdn)


def body(
    tokens,
    norm_gain,
    expert_gate,
    expert_up,
    expert_down,
    shared_gate,
    shared_up,
    shared_down,
    expert_ids,
    route_weights,
):
    gain = norm_gain[None, :, None]
    wgu = jnp.concatenate([expert_gate * gain, expert_up * gain], axis=2).astype(BF).reshape(NF, PER, KR, 2 * HC)
    wdn = expert_down.astype(BF).reshape(NF, PER, KD, DC)
    sgu = (jnp.concatenate([shared_gate, shared_up], axis=1) * norm_gain[:, None]).astype(BF)
    wide = tokens.astype(F32)
    normed = (wide * lax.rsqrt(jnp.mean(wide * wide, axis=-1, keepdims=True) + EPS)).astype(BF)
    mine = lax.dynamic_slice_in_dim(normed, lax.axis_index("tp") * DC, DC, 1)
    ids = jnp.pad(expert_ids.T, ((0, 16 - TOP_K), (0, DC - TOK)), constant_values=EXPERTS).astype(BF)
    tblk = jnp.concatenate([mine, sgu, shared_down.astype(BF), ids], axis=0)
    gu, dn, sw, ret, shared = exchange(tblk, normed, wgu, wdn)
    hit = expert_ids[:, :, None] == jnp.arange(EXPERTS, dtype=jnp.int32)
    match = jnp.sum(hit.astype(F32), axis=1)
    weight = jnp.sum(jnp.where(hit, route_weights[:, :, None], 0.0), axis=1)
    low = jnp.tril(jnp.ones((TOK, TOK), BF), -1)
    rank = jnp.dot(low, match.astype(BF), preferred_element_type=F32).astype(jnp.int32)
    mix = jnp.where(
        rank[:, :, None] == jnp.arange(CAP, dtype=jnp.int32), weight[:, :, None], 0.0
    ).reshape(TOK, EXPERTS * CAP)
    high = mix.astype(BF)
    rest = (mix - high.astype(F32)).astype(BF)
    rows = ret.reshape(EXPERTS * CAP, DC)
    routed = jnp.dot(high, rows, preferred_element_type=F32) + jnp.dot(rest, rows, preferred_element_type=F32)
    return (
        gu[:, :, :HC],
        gu[:, :, HC:],
        dn,
        sw[:, :KR, :HC].reshape(D, HC),
        sw[:, :KR, HC:].reshape(D, HC),
        sw[:, KR:, :].reshape(DE, DC),
        (shared + routed).astype(BF),
    )


def solution(mesh):
    in_specs = (
        P("fs", None),
        P("fs"),
        P(None, "fs", "tp"),
        P(None, "fs", "tp"),
        P(None, "fs", "tp"),
        P("fs", "tp"),
        P("fs", "tp"),
        P("fs", "tp"),
        P("fs", None),
        P("fs", None),
    )
    out_specs = (
        P("fs", None, "tp"),
        P("fs", None, "tp"),
        P("fs", None, "tp"),
        P(None, "tp"),
        P(None, "tp"),
        P(None, "tp"),
        P("fs", "tp"),
    )
    return jax.shard_map(body, mesh=mesh, in_specs=in_specs, out_specs=out_specs, check_vma=False)
```

```python
import jax
import jax.numpy as jnp
from jax import lax
from jax.experimental import pallas as pl
from jax.experimental.pallas import tpu as pltpu
from jax.sharding import PartitionSpec as P

EPS = 1e-06
NZ, NX, NY = 8, 4, 4
NF, NT = NZ * NX, NY * 2
D, DE, TOK, TOP_K, EXPERTS = 2048, 1024, 192, 8, 64
CAP = 2 * TOK * TOP_K // EXPERTS
PER = EXPERTS // NF
DC = D // NT
HC = DE // NT
KR, KD = D // NF, DE // NF
SRC = NX * CAP
ROW_EXPERTS = NX * PER
OFFS = (0, -1, 1, -2, 2, -3, 3, 4)
ORDER = (4, 3, 6, 5, 7, 2, 1, 0)
BF, F32 = jnp.bfloat16, jnp.float32
MESH = pl.DeviceIdType.MESH


def silu_mul(a, b):
    return (a * (1.0 / (1.0 + jnp.exp(-a)))) * b


def kernel(
    tokens, ids_in, rw_in, gain_in, sgate, sup, sdown, gate, up, down_w,
    gate_o, up_o, dn_o, sg_o, su_o, sd_o, mixed_o,
    fg, fu, fd, wgu, wdn, nfull, ta, tb, xg, gu, dn, hg, hs, og, wt, r1, pt, pr, mv,
    zr, xr, szr, sxr, br, bs, cr, cs, er, d1, dr, ss, lo, li,
):
    fs, tp = lax.axis_index("fs"), lax.axis_index("tp")
    z, x = fs // NX, lax.rem(fs, NX)
    y, c = tp // 2, lax.rem(tp, 2)

    def fsn(dz, dx):
        return lax.rem(z + dz + NZ, NZ) * NX + lax.rem(x + dx + NX, NX)

    def tpn(dy, dc):
        return lax.rem(y + dy + NY, NY) * 2 + lax.rem(c + dc, 2)

    yp, ym, sib = tpn(1, 0), tpn(-1, 0), tpn(0, 1)
    cols = pl.ds(pl.multiple_of(tp * DC, DC), DC)
    hcols = pl.ds(pl.multiple_of(tp * HC, HC), HC)

    def copy(src, dst, s, r, f, t):
        return pltpu.make_async_remote_copy(
            src_ref=src, dst_ref=dst, send_sem=s, recv_sem=r, device_id=(f, t), device_id_type=MESH
        )

    def arrived(dst, r):
        copy(dst, dst, ss.at[0], r, fs, sib).wait_recv()

    loads = [pltpu.make_async_copy(a, b, li.at[k]) for k, (a, b) in enumerate(((gate, fg), (up, fu), (down_w, fd)))]
    for load in loads:
        load.start()

    barrier = pltpu.get_barrier_semaphore()
    for k in range(1, NF):
        pl.semaphore_signal(barrier, inc=1, device_id=(lax.rem(fs + k, NF), tp), device_id_type=MESH)
    for t in (yp, ym, sib):
        pl.semaphore_signal(barrier, inc=1, device_id=(fs, t), device_id_type=MESH)

    wide = tokens[...].astype(F32)
    scale = lax.rsqrt(jnp.mean(wide * wide, axis=-1, keepdims=True) + EPS)
    nfull[...] = (wide * scale).astype(BF)
    ta[fs, pl.ds(0, TOK), :] = nfull[:, cols]
    ta[fs, pl.ds(TOK, 16), :] = jnp.zeros((16, DC), BF)
    ta[fs, pl.ds(TOK, 16), pl.ds(0, TOK)] = jnp.concatenate(
        [ids_in[...].astype(F32), rw_in[...]], axis=0
    ).astype(BF)
    diag = lax.broadcasted_iota(jnp.int32, (KR, KR), 0) == lax.broadcasted_iota(jnp.int32, (KR, KR), 1)
    gain = jnp.sum(jnp.where(diag, gain_in[...], 0.0), axis=1, keepdims=True)
    tb[fs, pl.ds(0, KR), pl.ds(0, HC)] = (sgate[...] * gain).astype(BF)
    tb[fs, pl.ds(0, KR), pl.ds(HC, HC)] = (sup[...] * gain).astype(BF)
    tb[fs, pl.ds(KR, KD), :] = sdown[...].astype(BF)
    pl.semaphore_wait(barrier, NF - 1 + 3)

    zp, zm, xp, xm = fsn(1, 0), fsn(-1, 0), fsn(0, 1), fsn(0, -1)

    def zi(i):
        return lax.rem(z + OFFS[i] + NZ, NZ)

    def z_step(buf, i, s, zq, xq):
        at_home = zi(i) * NX + x
        rows = buf.shape[1]
        cut = rows // 32 * 16
        blk = buf.at[at_home]
        low, high = buf.at[at_home, pl.ds(0, cut)], buf.at[at_home, pl.ds(cut, rows - cut)]
        if i == 0:
            copy(blk, blk, s, zq.at[1], zp, tp).start()
            copy(blk, blk, s, zq.at[2], zm, tp).start()
        elif i == 7:
            arrived(low, zq.at[7])
            arrived(high, zq.at[8])
        else:
            arrived(blk, zq.at[i])
            if i == 5:
                copy(low, low, s, zq.at[7], zp, tp).start()
            elif i == 6:
                copy(high, high, s, zq.at[8], zm, tp).start()
            else:
                copy(blk, blk, s, zq.at[i + 2], zp if OFFS[i] < 0 else zm, tp).start()
        copy(blk, blk, s, xq.at[i, 0], xp, tp).start()
        copy(blk, blk, s, xq.at[i, 1], xm, tp).start()

    def x_step(buf, i, s, zq, xq):
        rows = buf.shape[1]
        cut = rows // 32 * 16
        left = zi(i) * NX + lax.rem(x + NX - 1, NX)
        right = zi(i) * NX + lax.rem(x + 1, NX)
        arrived(buf.at[left], xq.at[i, 0])
        low = buf.at[left, pl.ds(0, cut)]
        copy(low, low, s, xq.at[i, 2], xp, tp).start()
        arrived(buf.at[right], xq.at[i, 1])
        high = buf.at[right, pl.ds(cut, rows - cut)]
        copy(high, high, s, xq.at[i, 3], xm, tp).start()

    def x_last(buf, i, s, zq, xq):
        rows = buf.shape[1]
        cut = rows // 32 * 16
        far = zi(i) * NX + lax.rem(x + 2, NX)
        arrived(buf.at[far, pl.ds(0, cut)], xq.at[i, 2])
        arrived(buf.at[far, pl.ds(cut, rows - cut)], xq.at[i, 3])

    slot = lax.broadcasted_iota(jnp.int32, (CAP, TOK), 0).astype(F32)

    def places(match):
        before = (
            lax.broadcasted_iota(jnp.int32, (TOK, TOK), 0) < lax.broadcasted_iota(jnp.int32, (TOK, TOK), 1)
        )
        upper = jnp.where(before, 1.0, 0.0).astype(BF)
        rank = jnp.dot(match.astype(BF), upper, preferred_element_type=F32)
        return jnp.where(match > 0.5, rank, -1.0)

    def select(i):
        first = (PER * fs).astype(F32)
        rows = []
        for k in range(NX):
            ids = ta[zi(i) * NX + k, pl.ds(TOK, 16), pl.ds(0, TOK)].astype(F32)[:TOP_K]
            for e in range(PER):
                rows.append(jnp.sum(jnp.where(ids == first + e, 1.0, 0.0), axis=0, keepdims=True))
        place = places(jnp.concatenate(rows, axis=0))
        for k in range(NX):
            hot = jnp.concatenate(
                [jnp.where(slot == place[PER * k + e : PER * k + e + 1], 1.0, 0.0) for e in range(PER)], axis=0
            ).astype(BF)
            rows = jnp.dot(hot, ta[zi(i) * NX + k, pl.ds(0, TOK), :], preferred_element_type=F32).astype(BF)
            for e in range(PER):
                xg[i, e, pl.ds(CAP * k, CAP), cols] = rows[CAP * e : CAP * (e + 1)]

    def weigh(i):
        both = ta[zi(i) * NX + x, pl.ds(TOK, 16), pl.ds(0, TOK)].astype(F32)
        ids, weights = both[:TOP_K], both[TOP_K:]
        first = (ROW_EXPERTS * z).astype(F32)
        hits, sums = [], []
        for e in range(ROW_EXPERTS):
            hit = ids == first + e
            hits.append(jnp.sum(jnp.where(hit, 1.0, 0.0), axis=0, keepdims=True))
            sums.append(jnp.sum(jnp.where(hit, weights, 0.0), axis=0, keepdims=True))
        place = places(jnp.concatenate(hits, axis=0))
        for e in range(ROW_EXPERTS):
            wt[i, pl.ds(CAP * e, CAP), :] = jnp.where(slot == place[e : e + 1], sums[e], 0.0).astype(BF)

    def at(buf, i, w, t):
        return buf.at[i, :, :, pl.ds(pl.multiple_of(t * w, w), w)]

    def half(buf, i, w, t, e):
        return buf.at[i, e, :, pl.ds(pl.multiple_of(t * w, w), w)]

    def tp_send(buf, i, w, s, r, b):
        own = at(buf, i, w, tp)
        copy(own, own, s, r.at[0], fs, yp).start()
        copy(own, own, s, r.at[1], fs, ym).start()
        copy(own, own, s, b, fs, sib).start()

    def tp_pass(buf, i, w, s, r, b):
        a = at(buf, i, w, ym)
        arrived(a, r.at[0])
        h = half(buf, i, w, ym, 0)
        copy(h, h, s, r.at[2], fs, yp).start()
        copy(a, a, s, b, fs, sib).start()
        a = at(buf, i, w, yp)
        arrived(a, r.at[1])
        h = half(buf, i, w, yp, 1)
        copy(h, h, s, r.at[3], fs, ym).start()
        copy(a, a, s, b, fs, sib).start()

    def tp_last(buf, i, w, s, r, b):
        far = tpn(2, 0)
        for e in range(2):
            h = half(buf, i, w, far, e)
            arrived(h, r.at[2 + e])
            copy(h, h, s, b, fs, sib).start()

    def tp_done(buf, i, w, b):
        arrived(buf.at[i, :, :, pl.ds(0, 4 * w)], b)

    peers = [(dz, dx) for dx in (0, 1, 3, 2) for dz in (1, -1, 2, -2, 3, -3, 4, 0)]
    peers = [p for p in peers if p != (0, 0)]
    gu_rows = pl.ds(pl.multiple_of(fs * KR, KR), KR)
    dn_rows = pl.ds(pl.multiple_of(fs * KD, KD), KD)

    def send_gu(n):
        f = fsn(*peers[n])
        copy(wgu.at[f], gu.at[:, gu_rows, :], ss.at[3], er.at[0], f, tp).start()

    def send_dn(n):
        f = fsn(*peers[n])
        copy(wdn.at[f], dn.at[:, dn_rows, :], ss.at[4], er.at[1], f, tp).start()

    def round_weights():
        for load in loads:
            load.wait()

        @pl.loop(0, NF)
        def _(f):
            for e in range(PER):
                wgu[f, e, :, :HC] = (fg[PER * f + e] * gain).astype(BF)
                wgu[f, e, :, HC:] = (fu[PER * f + e] * gain).astype(BF)
                wdn[f, e] = fd[PER * f + e].astype(BF)

        gu[:, gu_rows, :] = wgu[fs]
        dn[:, dn_rows, :] = wdn[fs]

    def gate_up(i):
        for e in range(PER):
            both = jnp.dot(xg[i, e], gu[e], preferred_element_type=F32)
            hg[i, e, :, hcols] = silu_mul(both[:, :HC], both[:, HC:]).astype(BF)

    def shared_gate_up():
        both = jnp.dot(nfull[...], tb[:, pl.ds(0, KR), :].reshape(D, 2 * HC), preferred_element_type=F32)
        mid = silu_mul(both[:, :HC], both[:, HC:]).astype(BF)
        hs[0, 0, :, hcols] = mid[: TOK // 2]
        hs[0, 1, :, hcols] = mid[TOK // 2 :]

    def down(i):
        for e in range(PER):
            out = jnp.dot(hg[i, e], dn[e], preferred_element_type=F32).astype(BF)
            for k in range(NX):
                og[i, k, pl.ds(CAP * e, CAP), :] = out[CAP * k : CAP * (k + 1)]

    def give_x(i):
        r1[i, x] = og[i, x]
        for dx in (1, 3, 2):
            k = lax.rem(x + dx, NX)
            copy(og.at[i, k], r1.at[i, x], ss.at[5], d1.at[i], fsn(0, dx), tp).start()

    def give_z(i):
        arrived(r1.at[i, pl.ds(0, NX - 1)], d1.at[i])
        part = lax.dot_general(
            wt[i], r1[i].reshape(NX * PER * CAP, DC), (((0,), (0,)), ((), ())), preferred_element_type=F32
        ).astype(BF)
        if i == 0:
            pr[z] = part
        else:
            pt[i] = part
            copy(pt.at[i], pr.at[z], ss.at[7], dr.at[0], zi(i) * NX + x, tp).start()

    tok = lambda i: (ta, i, ss.at[0], zr, xr)
    shr = lambda i: (tb, i, ss.at[8], szr, sxr)
    bq = lambda i: (xg, i, DC, ss.at[1], br.at[i], bs.at[i])
    cq = lambda i: (hg, i, HC, ss.at[2], cr.at[i], cs.at[i])
    shared = (hs, 0, HC, ss.at[6], cr.at[NZ], cs.at[NZ])
    outs = []

    def put(src, dst):
        outs.append(pltpu.make_async_copy(src, dst, lo.at[len(outs)]))
        outs[-1].start()

    def shared_gather(n):
        if 0 <= n < NZ:
            z_step(*shr(n))
        if 0 <= n - 1 < NZ:
            x_step(*shr(n - 1))
        if 0 <= n - 2 < NZ:
            x_last(*shr(n - 2))

    todo_gu, todo_dn = list(range(NF - 1)), list(range(NF - 1))
    FIRST = NZ + 4
    for tick in range(FIRST):
        if tick < NZ:
            z_step(*tok(tick))
        if 0 <= tick - 1 < NZ:
            x_step(*tok(tick - 1))
        if 0 <= tick - 2 < NZ:
            x_last(*tok(tick - 2))
            select(tick - 2)
            tp_send(*bq(tick - 2))
        if 0 <= tick - 3 < NZ:
            tp_pass(*bq(tick - 3))
        if 0 <= tick - 4 < NZ:
            tp_last(*bq(tick - 4))
        if tick == 0:
            round_weights()
        shared_gather(tick - NZ)
        for _ in range(3 if tick < NZ else 4):
            if todo_gu:
                send_gu(todo_gu.pop(0))
        if tick >= NZ + 2:
            for _ in range(8):
                if todo_dn:
                    send_dn(todo_dn.pop(0))
        if tick < NZ:
            weigh(tick)

    arrived(gu.at[:, pl.ds(0, D - KR), :], er.at[0])
    put(gu.at[:, :, pl.ds(0, HC)], gate_o)
    put(gu.at[:, :, pl.ds(HC, HC)], up_o)
    for tick in range(NZ + 5):
        if tick < NZ:
            i = ORDER[tick]
            tp_done(xg, i, DC, bs.at[i])
            gate_up(i)
            tp_send(*cq(i))
        if 0 <= tick - 1 < NZ:
            tp_pass(*cq(ORDER[tick - 1]))
        if 0 <= tick - 2 < NZ:
            tp_last(*cq(ORDER[tick - 2]))
        for _ in range(8):
            if todo_dn:
                send_dn(todo_dn.pop(0))
        n = tick + FIRST - NZ
        shared_gather(n)
        if n == NZ + 2:
            shared_gate_up()
            tp_send(*shared)
            put(tb.at[:, pl.ds(0, KR), pl.ds(0, HC)], sg_o)
            put(tb.at[:, pl.ds(0, KR), pl.ds(HC, HC)], su_o)
            put(tb.at[:, pl.ds(KR, KD), :], sd_o)
        elif n == NZ + 3:
            tp_pass(*shared)
        elif n == NZ + 4:
            tp_last(*shared)
        if 0 <= tick - 3 < NZ:
            i = ORDER[tick - 3]
            if tick == 3:
                arrived(dn.at[:, pl.ds(0, DE - KD), :], er.at[1])
                put(dn, dn_o)
            tp_done(hg, i, HC, cs.at[i])
            down(i)
            give_x(i)
        if 0 <= tick - 4 < NZ:
            give_z(ORDER[tick - 4])
    tp_done(hs, 0, HC, cs.at[NZ])
    sdn = tb[:, pl.ds(KR, KD), :].reshape(DE, DC)
    total = jnp.concatenate([jnp.dot(hs[0, e], sdn, preferred_element_type=F32) for e in range(2)], axis=0)
    arrived(pr.at[pl.ds(0, NZ - 1)], dr.at[0])
    for k in range(NZ):
        total = total + pr[k].astype(F32)
    mv[...] = total.astype(BF)
    put(mv, mixed_o)

    def sent(ref, s):
        copy(ref, ref, s, dr.at[0], fs, sib).wait_send()

    sent(ta.at[pl.ds(0, NF - 1)], ss.at[0])
    sent(tb.at[pl.ds(0, NF - 1)], ss.at[8])
    sent(xg.at[pl.ds(0, NZ - 1)], ss.at[1])
    sent(hg.at[pl.ds(0, NZ - 1)], ss.at[2])
    sent(gu.at[:, pl.ds(0, D - KR), :], ss.at[3])
    sent(dn.at[:, pl.ds(0, DE - KD), :], ss.at[4])
    sent(r1.at[:, pl.ds(0, NX - 1)], ss.at[5])
    sent(hs.at[0, :, :, pl.ds(0, 7 * HC)], ss.at[6])
    sent(pr.at[pl.ds(0, NZ - 1)], ss.at[7])
    for out in outs:
        out.wait()


def exchange(tokens, ids, rw, gain, sgate, sup, sdown, gate, up, down_w):
    vmem, anyw = pl.BlockSpec(memory_space=pltpu.VMEM), pl.BlockSpec(memory_space=pl.ANY)
    dma = pltpu.SemaphoreType.DMA
    return pl.pallas_call(
        kernel,
        out_shape=(
            jax.ShapeDtypeStruct((PER, D, HC), BF),
            jax.ShapeDtypeStruct((PER, D, HC), BF),
            jax.ShapeDtypeStruct((PER, DE, DC), BF),
            jax.ShapeDtypeStruct((NF, KR, HC), BF),
            jax.ShapeDtypeStruct((NF, KR, HC), BF),
            jax.ShapeDtypeStruct((NF, KD, DC), BF),
            jax.ShapeDtypeStruct((TOK, DC), BF),
        ),
        in_specs=[vmem] * 7 + [anyw] * 3,
        out_specs=(anyw,) * 7,
        scratch_shapes=[
            pltpu.VMEM((EXPERTS, KR, HC), F32),
            pltpu.VMEM((EXPERTS, KR, HC), F32),
            pltpu.VMEM((EXPERTS, KD, DC), F32),
            pltpu.VMEM((NF, PER, KR, 2 * HC), BF),
            pltpu.VMEM((NF, PER, KD, DC), BF),
            pltpu.VMEM((TOK, D), BF),
            pltpu.VMEM((NF, TOK + 16, DC), BF),
            pltpu.VMEM((NF, KR + KD, DC), BF),
            pltpu.VMEM((NZ, PER, SRC, D), BF),
            pltpu.VMEM((PER, D, 2 * HC), BF),
            pltpu.VMEM((PER, DE, DC), BF),
            pltpu.VMEM((NZ, PER, SRC, DE), BF),
            pltpu.VMEM((1, 2, TOK // 2, DE), BF),
            pltpu.VMEM((NZ, NX, PER * CAP, DC), BF),
            pltpu.VMEM((NZ, ROW_EXPERTS * CAP, TOK), BF),
            pltpu.VMEM((NZ, NX, PER * CAP, DC), BF),
            pltpu.VMEM((NZ, TOK, DC), BF),
            pltpu.VMEM((NZ, TOK, DC), BF),
            pltpu.VMEM((TOK, DC), BF),
            dma((9,)), dma((NZ, 4)), dma((9,)), dma((NZ, 4)), dma((NZ, 4)), dma((NZ,)), dma((NZ + 1, 4)),
            dma((NZ + 1,)), dma((2,)), dma((NZ,)), dma((1,)), dma((9,)), dma((7,)), dma((3,)),
        ],
        compiler_params=pltpu.CompilerParams(
            collective_id=0, has_side_effects=True, vmem_limit_bytes=60 * 1024 * 1024
        ),
    )(tokens, ids, rw, gain, sgate, sup, sdown, gate, up, down_w)


def writer(*refs):
    n = len(refs) // 2
    sems = refs[-1]
    copies = [pltpu.make_async_copy(a, b, sems.at[k]) for k, (a, b) in enumerate(zip(refs[:n], refs[n : 2 * n]))]
    for one in copies:
        one.start()
    for one in copies:
        one.wait()


def write_out(*arrays):
    return pl.pallas_call(
        writer,
        out_shape=tuple(jax.ShapeDtypeStruct(a.shape, a.dtype) for a in arrays),
        in_specs=[pl.BlockSpec(memory_space=pltpu.VMEM)] * len(arrays),
        out_specs=(pl.BlockSpec(memory_space=pl.ANY),) * len(arrays),
        scratch_shapes=[pltpu.SemaphoreType.DMA((len(arrays),))],
        compiler_params=pltpu.CompilerParams(vmem_limit_bytes=8 * 1024 * 1024),
    )(*arrays)


def body(
    tokens,
    norm_gain,
    expert_gate,
    expert_up,
    expert_down,
    shared_gate,
    shared_up,
    shared_down,
    expert_ids,
    route_weights,
):
    results = exchange(
        tokens, expert_ids.T, route_weights.T, norm_gain[None], shared_gate, shared_up, shared_down,
        expert_gate, expert_up, expert_down,
    )
    gate_ready, up_ready, down_ready, sg, su, sd, mixed = write_out(*results)
    return (
        gate_ready,
        up_ready,
        down_ready,
        sg.reshape(D, HC),
        su.reshape(D, HC),
        sd.reshape(DE, DC),
        mixed,
    )


def solution(mesh):
    in_specs = (
        P("fs", None),
        P("fs"),
        P(None, "fs", "tp"),
        P(None, "fs", "tp"),
        P(None, "fs", "tp"),
        P("fs", "tp"),
        P("fs", "tp"),
        P("fs", "tp"),
        P("fs", None),
        P("fs", None),
    )
    out_specs = (
        P("fs", None, "tp"),
        P("fs", None, "tp"),
        P("fs", None, "tp"),
        P(None, "tp"),
        P(None, "tp"),
        P(None, "tp"),
        P("fs", "tp"),
    )
    return jax.shard_map(body, mesh=mesh, in_specs=in_specs, out_specs=out_specs, check_vma=False)
```

```python
import jax
import jax.numpy as jnp
from jax import lax
from jax.experimental import pallas as pl
from jax.experimental.pallas import tpu as pltpu
from jax.sharding import PartitionSpec as P

EPS = 1e-06
NZ, NX, NY = 8, 4, 4
NF, NT = NZ * NX, NY * 2
D, DE, TOK, TOP_K, EXPERTS = 2048, 1024, 192, 8, 64
CAP = 2 * TOK * TOP_K // EXPERTS
PER = EXPERTS // NF
DC = D // NT
HC = DE // NT
KR, KD = D // NF, DE // NF
SRC = NX * CAP
ROW_EXPERTS = NX * PER
OFFS = (0, -1, 1, -2, 2, -3, 3, 4)
ORDER = (5, 7, 3, 6, 1, 4, 0, 2)
SECOND = 10
SHARED = 6
LAG = 3
FEED = (1, 1, 1, 1, 0)
BF, F32 = jnp.bfloat16, jnp.float32
MESH = pl.DeviceIdType.MESH


def silu_mul(a, b):
    return (a * (1.0 / (1.0 + jnp.exp(-a)))) * b


def kernel(
    tokens, ids_in, rw_in, gain_in, sgate, sup, sdown, gate, up, down_w,
    gu, dn, tb, mv,
    fg, fu, fd, wgu, wdn, nfull, ta, xg, hg, hs, og, wt, r1, pt, pr, po, sh,
    zr, xr, szr, sxr, br, bs, cr, cs, er, d1, dr, ss, li,
):
    fs, tp = lax.axis_index("fs"), lax.axis_index("tp")
    z, x = fs // NX, lax.rem(fs, NX)
    y, c = tp // 2, lax.rem(tp, 2)

    def fsn(dz, dx):
        return lax.rem(z + dz + NZ, NZ) * NX + lax.rem(x + dx + NX, NX)

    def tpn(dy, dc):
        return lax.rem(y + dy + NY, NY) * 2 + lax.rem(c + dc, 2)

    yp, ym, sib = tpn(1, 0), tpn(-1, 0), tpn(0, 1)
    cols = pl.ds(pl.multiple_of(tp * DC, DC), DC)
    hcols = pl.ds(pl.multiple_of(tp * HC, HC), HC)

    def copy(src, dst, s, r, f, t):
        return pltpu.make_async_remote_copy(
            src_ref=src, dst_ref=dst, send_sem=s, recv_sem=r, device_id=(f, t), device_id_type=MESH
        )

    def arrived(dst, r):
        copy(dst, dst, ss.at[0], r, fs, sib).wait_recv()

    loads = [pltpu.make_async_copy(a, b, li.at[k]) for k, (a, b) in enumerate(((gate, fg), (up, fu), (down_w, fd)))]
    for load in loads:
        load.start()

    barrier = pltpu.get_barrier_semaphore()
    for k in range(1, NF):
        pl.semaphore_signal(barrier, inc=1, device_id=(lax.rem(fs + k, NF), tp), device_id_type=MESH)
    for t in (yp, ym, sib):
        pl.semaphore_signal(barrier, inc=1, device_id=(fs, t), device_id_type=MESH)

    wide = tokens[...].astype(F32)
    scale = lax.rsqrt(jnp.mean(wide * wide, axis=-1, keepdims=True) + EPS)
    nfull[...] = (wide * scale).astype(BF)
    ta[fs, pl.ds(0, TOK), :] = nfull[:, cols]
    ta[fs, pl.ds(TOK, 16), :] = jnp.zeros((16, DC), BF)
    ta[fs, pl.ds(TOK, 16), pl.ds(0, TOK)] = jnp.concatenate(
        [ids_in[...].astype(F32), rw_in[...]], axis=0
    ).astype(BF)
    diag = lax.broadcasted_iota(jnp.int32, (KR, KR), 0) == lax.broadcasted_iota(jnp.int32, (KR, KR), 1)
    gain = jnp.sum(jnp.where(diag, gain_in[...], 0.0), axis=1, keepdims=True)
    tb[fs, pl.ds(0, KR), pl.ds(0, HC)] = (sgate[...] * gain).astype(BF)
    tb[fs, pl.ds(0, KR), pl.ds(HC, HC)] = (sup[...] * gain).astype(BF)
    tb[fs, pl.ds(KR, KD), :] = sdown[...].astype(BF)
    pl.semaphore_wait(barrier, NF - 1 + 3)

    zp, zm, xp, xm = fsn(1, 0), fsn(-1, 0), fsn(0, 1), fsn(0, -1)

    def zi(i):
        return lax.rem(z + OFFS[i] + NZ, NZ)

    def z_step(buf, i, s, zq, xq):
        at_home = zi(i) * NX + x
        rows = buf.shape[1]
        cut = rows // 32 * 16
        blk = buf.at[at_home]
        low, high = buf.at[at_home, pl.ds(0, cut)], buf.at[at_home, pl.ds(cut, rows - cut)]
        if i == 0:
            copy(blk, blk, s, zq.at[1], zp, tp).start()
            copy(blk, blk, s, zq.at[2], zm, tp).start()
        elif i == 7:
            arrived(low, zq.at[7])
            arrived(high, zq.at[8])
        else:
            arrived(blk, zq.at[i])
            if i == 5:
                copy(low, low, s, zq.at[7], zp, tp).start()
            elif i == 6:
                copy(high, high, s, zq.at[8], zm, tp).start()
            else:
                copy(blk, blk, s, zq.at[i + 2], zp if OFFS[i] < 0 else zm, tp).start()
        copy(blk, blk, s, xq.at[i, 0], xp, tp).start()
        copy(blk, blk, s, xq.at[i, 1], xm, tp).start()

    def x_step(buf, i, s, zq, xq):
        rows = buf.shape[1]
        cut = rows // 32 * 16
        left = zi(i) * NX + lax.rem(x + NX - 1, NX)
        right = zi(i) * NX + lax.rem(x + 1, NX)
        arrived(buf.at[left], xq.at[i, 0])
        low = buf.at[left, pl.ds(0, cut)]
        copy(low, low, s, xq.at[i, 2], xp, tp).start()
        arrived(buf.at[right], xq.at[i, 1])
        high = buf.at[right, pl.ds(cut, rows - cut)]
        copy(high, high, s, xq.at[i, 3], xm, tp).start()

    def x_last(buf, i, s, zq, xq):
        rows = buf.shape[1]
        cut = rows // 32 * 16
        far = zi(i) * NX + lax.rem(x + 2, NX)
        arrived(buf.at[far, pl.ds(0, cut)], xq.at[i, 2])
        arrived(buf.at[far, pl.ds(cut, rows - cut)], xq.at[i, 3])

    slot = lax.broadcasted_iota(jnp.int32, (CAP, TOK), 0).astype(F32)

    def places(match):
        before = (
            lax.broadcasted_iota(jnp.int32, (TOK, TOK), 0) < lax.broadcasted_iota(jnp.int32, (TOK, TOK), 1)
        )
        upper = jnp.where(before, 1.0, 0.0).astype(BF)
        rank = jnp.dot(match.astype(BF), upper, preferred_element_type=F32)
        return jnp.where(match > 0.5, rank, -1.0)

    def select(i):
        first = (PER * fs).astype(F32)
        rows = []
        for k in range(NX):
            ids = ta[zi(i) * NX + k, pl.ds(TOK, 16), pl.ds(0, TOK)].astype(F32)[:TOP_K]
            for e in range(PER):
                rows.append(jnp.sum(jnp.where(ids == first + e, 1.0, 0.0), axis=0, keepdims=True))
        place = places(jnp.concatenate(rows, axis=0))
        for k in range(NX):
            hot = jnp.concatenate(
                [jnp.where(slot == place[PER * k + e : PER * k + e + 1], 1.0, 0.0) for e in range(PER)], axis=0
            ).astype(BF)
            rows = jnp.dot(hot, ta[zi(i) * NX + k, pl.ds(0, TOK), :], preferred_element_type=F32).astype(BF)
            for e in range(PER):
                xg[i, e, pl.ds(CAP * k, CAP), cols] = rows[CAP * e : CAP * (e + 1)]

    def weigh(i):
        both = ta[zi(i) * NX + x, pl.ds(TOK, 16), pl.ds(0, TOK)].astype(F32)
        ids, weights = both[:TOP_K], both[TOP_K:]
        first = (ROW_EXPERTS * z).astype(F32)
        hits, sums = [], []
        for e in range(ROW_EXPERTS):
            hit = ids == first + e
            hits.append(jnp.sum(jnp.where(hit, 1.0, 0.0), axis=0, keepdims=True))
            sums.append(jnp.sum(jnp.where(hit, weights, 0.0), axis=0, keepdims=True))
        place = places(jnp.concatenate(hits, axis=0))
        for e in range(ROW_EXPERTS):
            wt[i, pl.ds(CAP * e, CAP), :] = jnp.where(slot == place[e : e + 1], sums[e], 0.0).astype(BF)

    def at(buf, i, w, t):
        return buf.at[i, :, :, pl.ds(pl.multiple_of(t * w, w), w)]

    def half(buf, i, w, t, e):
        return buf.at[i, e, :, pl.ds(pl.multiple_of(t * w, w), w)]

    def tp_send(buf, i, w, s, r, b):
        own = at(buf, i, w, tp)
        copy(own, own, s, r.at[0], fs, yp).start()
        copy(own, own, s, r.at[1], fs, ym).start()
        copy(own, own, s, b, fs, sib).start()

    def tp_pass(buf, i, w, s, r, b):
        a = at(buf, i, w, ym)
        arrived(a, r.at[0])
        h = half(buf, i, w, ym, 0)
        copy(h, h, s, r.at[2], fs, yp).start()
        copy(a, a, s, b, fs, sib).start()
        a = at(buf, i, w, yp)
        arrived(a, r.at[1])
        h = half(buf, i, w, yp, 1)
        copy(h, h, s, r.at[3], fs, ym).start()
        copy(a, a, s, b, fs, sib).start()

    def tp_last(buf, i, w, s, r, b):
        far = tpn(2, 0)
        for e in range(2):
            h = half(buf, i, w, far, e)
            arrived(h, r.at[2 + e])
            copy(h, h, s, b, fs, sib).start()

    def tp_done(buf, i, w, b):
        arrived(buf.at[i, :, :, pl.ds(0, 4 * w)], b)

    zs = (1, -1, 2, -2, 3, -3, 4, 0)
    peers = [(zs[(a + 2 * b) % NZ], (0, 1, 3, 2)[b]) for a in range(NZ) for b in range(NX)]
    peers = [p for p in peers if p != (0, 0)]
    gu_rows = pl.ds(pl.multiple_of(fs * KR, KR), KR)
    dn_rows = pl.ds(pl.multiple_of(fs * KD, KD), KD)

    def send_gu(n):
        f = fsn(*peers[n])
        copy(wgu.at[f], gu.at[:, gu_rows, :], ss.at[3], er.at[0], f, tp).start()

    def send_dn(n):
        f = fsn(*peers[n])
        copy(wdn.at[f], dn.at[:, dn_rows, :], ss.at[4], er.at[1], f, tp).start()

    def round_weights():
        for load in loads:
            load.wait()

        @pl.loop(0, NF)
        def _(f):
            for e in range(PER):
                wgu[f, e, :, :HC] = (fg[PER * f + e] * gain).astype(BF)
                wgu[f, e, :, HC:] = (fu[PER * f + e] * gain).astype(BF)
                wdn[f, e] = fd[PER * f + e].astype(BF)

        gu[:, gu_rows, :] = wgu[fs]
        dn[:, dn_rows, :] = wdn[fs]

    def gate_up(i):
        for e in range(PER):
            both = jnp.dot(xg[i, e], gu[e], preferred_element_type=F32)
            hg[i, e, :, hcols] = silu_mul(both[:, :HC], both[:, HC:]).astype(BF)

    def shared_gate_up():
        both = jnp.dot(nfull[...], tb[:, pl.ds(0, KR), :].reshape(D, 2 * HC), preferred_element_type=F32)
        mid = silu_mul(both[:, :HC], both[:, HC:]).astype(BF)
        hs[0, 0, :, hcols] = mid[: TOK // 2]
        hs[0, 1, :, hcols] = mid[TOK // 2 :]

    def down(i):
        for e in range(PER):
            out = jnp.dot(hg[i, e], dn[e], preferred_element_type=F32).astype(BF)
            for k in range(NX):
                og[i, k, pl.ds(CAP * e, CAP), :] = out[CAP * k : CAP * (k + 1)]

    def give_x(i):
        r1[i, x] = og[i, x]
        for dx in (1, 3, 2):
            k = lax.rem(x + dx, NX)
            copy(og.at[i, k], r1.at[i, x], ss.at[5], d1.at[i], fsn(0, dx), tp).start()

    def give_z(i):
        arrived(r1.at[i, pl.ds(0, NX - 1)], d1.at[i])
        part = lax.dot_general(
            wt[i], r1[i].reshape(NX * PER * CAP, DC), (((0,), (0,)), ((), ())), preferred_element_type=F32
        )
        d = OFFS[i]
        if d == 0:
            po[...] = part
            return
        far, base = (4, 0) if d > 0 else (3, 4)
        k = base + abs(d)
        if abs(d) < far:
            arrived(pr.at[k], dr.at[k])
            part = part + pr[k].astype(F32)
        pt[i] = part.astype(BF)
        copy(pt.at[i], pr.at[k - 1], ss.at[7], dr.at[k - 1], zp if d > 0 else zm, tp).start()

    tok = lambda i: (ta, i, ss.at[0], zr, xr)
    shr = lambda i: (tb, i, ss.at[8], szr, sxr)
    bq = lambda i: (xg, i, DC, ss.at[1], br.at[i], bs.at[i])
    cq = lambda i: (hg, i, HC, ss.at[2], cr.at[i], cs.at[i])
    shared = (hs, 0, HC, ss.at[6], cr.at[NZ], cs.at[NZ])

    def shared_gather(n):
        if 0 <= n < NZ:
            z_step(*shr(n))
        if 0 <= n - 1 < NZ:
            x_step(*shr(n - 1))
        if 0 <= n - 2 < NZ:
            x_last(*shr(n - 2))

    todo = [(send_gu, n) for n in range(NF - 1)] + [(send_dn, n) for n in range(NF - 1)]

    def flush(keep):
        while len(todo) > keep:
            send, n = todo.pop(0)
            send(n)

    def feed(k):
        flush(len(todo) - min(FEED[k] if len(todo) >= NF else 2 * FEED[k], len(todo)))

    for tick in range(SECOND + NZ + LAG + 2):
        if tick < NZ:
            z_step(*tok(tick))
        if tick == 0:
            round_weights()
        feed(0)
        if 0 <= tick - 1 < NZ:
            x_step(*tok(tick - 1))
        feed(1)
        if 0 <= tick - 2 < NZ:
            x_last(*tok(tick - 2))
            select(tick - 2)
            tp_send(*bq(tick - 2))
        feed(2)
        if 0 <= tick - 3 < NZ:
            tp_pass(*bq(tick - 3))
        feed(3)
        if 0 <= tick - 4 < NZ:
            tp_last(*bq(tick - 4))
        feed(4)
        shared_gather(tick - SHARED)
        if tick < NZ:
            weigh(tick)
        t = tick - SECOND
        if t == 0:
            flush(NF - 1)
            arrived(gu.at[:, pl.ds(0, D - KR), :], er.at[0])
        if 0 <= t < NZ:
            i = ORDER[t]
            tp_done(xg, i, DC, bs.at[i])
            gate_up(i)
            tp_send(*cq(i))
        if 0 <= t - 1 < NZ:
            tp_pass(*cq(ORDER[t - 1]))
        if 0 <= t - 2 < NZ:
            tp_last(*cq(ORDER[t - 2]))
        n = tick - SHARED - NZ
        if n == 2:
            shared_gate_up()
            tp_send(*shared)
        elif n == 3:
            tp_pass(*shared)
        elif n == 4:
            tp_last(*shared)
        if 0 <= t - LAG < NZ:
            i = ORDER[t - LAG]
            if t == LAG:
                flush(0)
                arrived(dn.at[:, pl.ds(0, DE - KD), :], er.at[1])
            tp_done(hg, i, HC, cs.at[i])
            down(i)
            give_x(i)
        if 0 <= t - LAG - 1 < NZ:
            give_z(ORDER[t - LAG - 1])
        if t == NZ + 1:
            tp_done(hs, 0, HC, cs.at[NZ])
            sdn = tb[:, pl.ds(KR, KD), :].reshape(DE, DC)
            for e in range(2):
                sh[pl.ds(e * (TOK // 2), TOK // 2), :] = jnp.dot(hs[0, e], sdn, preferred_element_type=F32)
    total = sh[...] + po[...]
    for k in (4, 0):
        arrived(pr.at[k], dr.at[k])
        total = total + pr[k].astype(F32)
    mv[...] = total.astype(BF)

    def sent(ref, s):
        copy(ref, ref, s, dr.at[0], fs, sib).wait_send()

    sent(ta.at[pl.ds(0, NF - 1)], ss.at[0])
    sent(tb.at[pl.ds(0, NF - 1)], ss.at[8])
    sent(xg.at[pl.ds(0, NZ - 1)], ss.at[1])
    sent(hg.at[pl.ds(0, NZ - 1)], ss.at[2])
    sent(gu.at[:, pl.ds(0, D - KR), :], ss.at[3])
    sent(dn.at[:, pl.ds(0, DE - KD), :], ss.at[4])
    sent(r1.at[:, pl.ds(0, NX - 1)], ss.at[5])
    sent(hs.at[0, :, :, pl.ds(0, 7 * HC)], ss.at[6])
    sent(pr.at[pl.ds(0, NZ - 1)], ss.at[7])


def exchange(tokens, ids, rw, gain, sgate, sup, sdown, gate, up, down_w):
    vmem, anyw = pl.BlockSpec(memory_space=pltpu.VMEM), pl.BlockSpec(memory_space=pl.ANY)
    dma = pltpu.SemaphoreType.DMA
    return pl.pallas_call(
        kernel,
        out_shape=(
            pltpu.VMEM((PER, D, 2 * HC), BF),
            pltpu.VMEM((PER, DE, DC), BF),
            pltpu.VMEM((NF, KR + KD, DC), BF),
            pltpu.VMEM((TOK, DC), BF),
        ),
        in_specs=[vmem] * 7 + [anyw] * 3,
        out_specs=(vmem,) * 4,
        scratch_shapes=[
            pltpu.VMEM((EXPERTS, KR, HC), F32),
            pltpu.VMEM((EXPERTS, KR, HC), F32),
            pltpu.VMEM((EXPERTS, KD, DC), F32),
            pltpu.VMEM((NF, PER, KR, 2 * HC), BF),
            pltpu.VMEM((NF, PER, KD, DC), BF),
            pltpu.VMEM((TOK, D), BF),
            pltpu.VMEM((NF, TOK + 16, DC), BF),
            pltpu.VMEM((NZ, PER, SRC, D), BF),
            pltpu.VMEM((NZ, PER, SRC, DE), BF),
            pltpu.VMEM((1, 2, TOK // 2, DE), BF),
            pltpu.VMEM((NZ, NX, PER * CAP, DC), BF),
            pltpu.VMEM((NZ, ROW_EXPERTS * CAP, TOK), BF),
            pltpu.VMEM((NZ, NX, PER * CAP, DC), BF),
            pltpu.VMEM((NZ, TOK, DC), BF),
            pltpu.VMEM((NZ - 1, TOK, DC), BF),
            pltpu.VMEM((TOK, DC), F32),
            pltpu.VMEM((TOK, DC), F32),
            dma((9,)), dma((NZ, 4)), dma((9,)), dma((NZ, 4)), dma((NZ, 4)), dma((NZ,)), dma((NZ + 1, 4)),
            dma((NZ + 1,)), dma((2,)), dma((NZ,)), dma((NZ - 1,)), dma((9,)), dma((3,)),
        ],
        compiler_params=pltpu.CompilerParams(
            collective_id=0, has_side_effects=True, vmem_limit_bytes=54 * 1024 * 1024
        ),
    )(tokens, ids, rw, gain, sgate, sup, sdown, gate, up, down_w)


def writer(gu, dn, tb, mv, gate_o, up_o, dn_o, sg_o, su_o, sd_o, mixed_o, sems):
    left, right = pl.ds(0, HC), pl.ds(HC, HC)
    pairs = (
        (gu.at[:, :, left], gate_o),
        (gu.at[:, :, right], up_o),
        (dn, dn_o),
        (tb.at[:, pl.ds(0, KR), left], sg_o),
        (tb.at[:, pl.ds(0, KR), right], su_o),
        (tb.at[:, pl.ds(KR, KD), :], sd_o),
        (mv, mixed_o),
    )
    copies = [pltpu.make_async_copy(a, b, sems.at[k]) for k, (a, b) in enumerate(pairs)]
    for one in copies:
        one.start()
    for one in copies:
        one.wait()


def write_out(*arrays):
    shapes = ((PER, D, HC), (PER, D, HC), (PER, DE, DC), (NF, KR, HC), (NF, KR, HC), (NF, KD, DC), (TOK, DC))
    return pl.pallas_call(
        writer,
        out_shape=tuple(jax.ShapeDtypeStruct(s, BF) for s in shapes),
        in_specs=[pl.BlockSpec(memory_space=pltpu.VMEM)] * len(arrays),
        out_specs=(pl.BlockSpec(memory_space=pl.ANY),) * len(shapes),
        scratch_shapes=[pltpu.SemaphoreType.DMA((len(shapes),))],
        compiler_params=pltpu.CompilerParams(vmem_limit_bytes=8 * 1024 * 1024),
    )(*arrays)


def body(
    tokens,
    norm_gain,
    expert_gate,
    expert_up,
    expert_down,
    shared_gate,
    shared_up,
    shared_down,
    expert_ids,
    route_weights,
):
    results = exchange(
        tokens, expert_ids.T, route_weights.T, norm_gain[None], shared_gate, shared_up, shared_down,
        expert_gate, expert_up, expert_down,
    )
    gate_ready, up_ready, down_ready, sg, su, sd, mixed = write_out(*results)
    return (
        gate_ready,
        up_ready,
        down_ready,
        sg.reshape(D, HC),
        su.reshape(D, HC),
        sd.reshape(DE, DC),
        mixed,
    )


def solution(mesh):
    in_specs = (
        P("fs", None),
        P("fs"),
        P(None, "fs", "tp"),
        P(None, "fs", "tp"),
        P(None, "fs", "tp"),
        P("fs", "tp"),
        P("fs", "tp"),
        P("fs", "tp"),
        P("fs", None),
        P("fs", None),
    )
    out_specs = (
        P("fs", None, "tp"),
        P("fs", None, "tp"),
        P("fs", None, "tp"),
        P(None, "tp"),
        P(None, "tp"),
        P(None, "tp"),
        P("fs", "tp"),
    )
    return jax.shard_map(body, mesh=mesh, in_specs=in_specs, out_specs=out_specs, check_vma=False)
```

```python
import jax
import jax.numpy as jnp
from jax import lax
from jax.experimental import pallas as pl
from jax.experimental.pallas import tpu as pltpu
from jax.sharding import PartitionSpec as P

EPS = 1e-06
NZ, NX, NY = 8, 4, 4
NF, NT = NZ * NX, NY * 2
D, DE, TOK, TOP_K, EXPERTS = 2048, 1024, 192, 8, 64
CAP = 2 * TOK * TOP_K // EXPERTS
PER = EXPERTS // NF
DC = D // NT
HC = DE // NT
KR, KD = D // NF, DE // NF
SRC = NX * CAP
ROW_EXPERTS = NX * PER
OFFS = (0, -1, 1, -2, 2, -3, 3, 4)
ORDER = (5, 7, 3, 6, 1, 4, 0, 2)
SECOND = 10
SHARED = 6
LAG = 3
FEED = (1, 1, 1, 1, 0)
BF, F32 = jnp.bfloat16, jnp.float32
MESH = pl.DeviceIdType.MESH


def silu_mul(a, b):
    return (a * (1.0 / (1.0 + jnp.exp(-a)))) * b


def kernel(
    tokens_h, ids_h, rw_h, gain_h, sgate_h, sup_h, sdown_h, gate, up, down_w,
    gu, dn, tb, mv,
    tokens, ids_in, rw_in, gain_in, sgate, sup, sdown,
    fg, fu, fd, wgu, wdn, nfull, ta, xg, hg, hs, og, wt, r1, pt, pr, po, sh,
    zr, xr, szr, sxr, br, bs, cr, cs, er, d1, dr, ss, li,
):
    fs, tp = lax.axis_index("fs"), lax.axis_index("tp")
    z, x = fs // NX, lax.rem(fs, NX)
    y, c = tp // 2, lax.rem(tp, 2)

    def fsn(dz, dx):
        return lax.rem(z + dz + NZ, NZ) * NX + lax.rem(x + dx + NX, NX)

    def tpn(dy, dc):
        return lax.rem(y + dy + NY, NY) * 2 + lax.rem(c + dc, 2)

    yp, ym, sib = tpn(1, 0), tpn(-1, 0), tpn(0, 1)
    cols = pl.ds(pl.multiple_of(tp * DC, DC), DC)
    hcols = pl.ds(pl.multiple_of(tp * HC, HC), HC)

    def copy(src, dst, s, r, f, t):
        return pltpu.make_async_remote_copy(
            src_ref=src, dst_ref=dst, send_sem=s, recv_sem=r, device_id=(f, t), device_id_type=MESH
        )

    def arrived(dst, r):
        copy(dst, dst, ss.at[0], r, fs, sib).wait_recv()

    small = (
        (tokens_h, tokens), (ids_h, ids_in), (rw_h, rw_in), (gain_h, gain_in),
        (sgate_h, sgate), (sup_h, sup), (sdown_h, sdown),
    )
    large = ((gate, fg), (up, fu), (down_w, fd))
    copies = [pltpu.make_async_copy(a, b, li.at[k]) for k, (a, b) in enumerate(small + large)]
    first, loads = copies[: len(small)], copies[len(small) :]
    for load in copies:
        load.start()

    barrier = pltpu.get_barrier_semaphore()
    for k in range(1, NF):
        pl.semaphore_signal(barrier, inc=1, device_id=(lax.rem(fs + k, NF), tp), device_id_type=MESH)
    for t in (yp, ym, sib):
        pl.semaphore_signal(barrier, inc=1, device_id=(fs, t), device_id_type=MESH)

    for load in first:
        load.wait()
    wide = tokens[...].astype(F32)
    scale = lax.rsqrt(jnp.mean(wide * wide, axis=-1, keepdims=True) + EPS)
    nfull[...] = (wide * scale).astype(BF)
    ta[fs, pl.ds(0, TOK), :] = nfull[:, cols]
    ta[fs, pl.ds(TOK, 16), :] = jnp.zeros((16, DC), BF)
    ta[fs, pl.ds(TOK, 16), pl.ds(0, TOK)] = jnp.concatenate(
        [ids_in[...].astype(F32), rw_in[...]], axis=0
    ).astype(BF)
    diag = lax.broadcasted_iota(jnp.int32, (KR, KR), 0) == lax.broadcasted_iota(jnp.int32, (KR, KR), 1)
    gain = jnp.sum(jnp.where(diag, gain_in[...], 0.0), axis=1, keepdims=True)
    tb[fs, pl.ds(0, KR), pl.ds(0, HC)] = (sgate[...] * gain).astype(BF)
    tb[fs, pl.ds(0, KR), pl.ds(HC, HC)] = (sup[...] * gain).astype(BF)
    tb[fs, pl.ds(KR, KD), :] = sdown[...].astype(BF)
    pl.semaphore_wait(barrier, NF - 1 + 3)

    zp, zm, xp, xm = fsn(1, 0), fsn(-1, 0), fsn(0, 1), fsn(0, -1)

    def zi(i):
        return lax.rem(z + OFFS[i] + NZ, NZ)

    def z_step(buf, i, s, zq, xq):
        at_home = zi(i) * NX + x
        rows = buf.shape[1]
        cut = rows // 32 * 16
        blk = buf.at[at_home]
        low, high = buf.at[at_home, pl.ds(0, cut)], buf.at[at_home, pl.ds(cut, rows - cut)]
        if i == 0:
            copy(blk, blk, s, zq.at[1], zp, tp).start()
            copy(blk, blk, s, zq.at[2], zm, tp).start()
        elif i == 7:
            arrived(low, zq.at[7])
            arrived(high, zq.at[8])
        else:
            arrived(blk, zq.at[i])
            if i == 5:
                copy(low, low, s, zq.at[7], zp, tp).start()
            elif i == 6:
                copy(high, high, s, zq.at[8], zm, tp).start()
            else:
                copy(blk, blk, s, zq.at[i + 2], zp if OFFS[i] < 0 else zm, tp).start()
        copy(blk, blk, s, xq.at[i, 0], xp, tp).start()
        copy(blk, blk, s, xq.at[i, 1], xm, tp).start()

    def x_step(buf, i, s, zq, xq):
        rows = buf.shape[1]
        cut = rows // 32 * 16
        left = zi(i) * NX + lax.rem(x + NX - 1, NX)
        right = zi(i) * NX + lax.rem(x + 1, NX)
        arrived(buf.at[left], xq.at[i, 0])
        low = buf.at[left, pl.ds(0, cut)]
        copy(low, low, s, xq.at[i, 2], xp, tp).start()
        arrived(buf.at[right], xq.at[i, 1])
        high = buf.at[right, pl.ds(cut, rows - cut)]
        copy(high, high, s, xq.at[i, 3], xm, tp).start()

    def x_last(buf, i, s, zq, xq):
        rows = buf.shape[1]
        cut = rows // 32 * 16
        far = zi(i) * NX + lax.rem(x + 2, NX)
        arrived(buf.at[far, pl.ds(0, cut)], xq.at[i, 2])
        arrived(buf.at[far, pl.ds(cut, rows - cut)], xq.at[i, 3])

    slot = lax.broadcasted_iota(jnp.int32, (CAP, TOK), 0).astype(F32)

    def places(match):
        before = (
            lax.broadcasted_iota(jnp.int32, (TOK, TOK), 0) < lax.broadcasted_iota(jnp.int32, (TOK, TOK), 1)
        )
        upper = jnp.where(before, 1.0, 0.0).astype(BF)
        rank = jnp.dot(match.astype(BF), upper, preferred_element_type=F32)
        return jnp.where(match > 0.5, rank, -1.0)

    def select(i):
        first = (PER * fs).astype(F32)
        rows = []
        for k in range(NX):
            ids = ta[zi(i) * NX + k, pl.ds(TOK, 16), pl.ds(0, TOK)].astype(F32)[:TOP_K]
            for e in range(PER):
                rows.append(jnp.sum(jnp.where(ids == first + e, 1.0, 0.0), axis=0, keepdims=True))
        place = places(jnp.concatenate(rows, axis=0))
        for k in range(NX):
            hot = jnp.concatenate(
                [jnp.where(slot == place[PER * k + e : PER * k + e + 1], 1.0, 0.0) for e in range(PER)], axis=0
            ).astype(BF)
            rows = jnp.dot(hot, ta[zi(i) * NX + k, pl.ds(0, TOK), :], preferred_element_type=F32).astype(BF)
            for e in range(PER):
                xg[i, e, pl.ds(CAP * k, CAP), cols] = rows[CAP * e : CAP * (e + 1)]

    def weigh(i):
        both = ta[zi(i) * NX + x, pl.ds(TOK, 16), pl.ds(0, TOK)].astype(F32)
        ids, weights = both[:TOP_K], both[TOP_K:]
        first = (ROW_EXPERTS * z).astype(F32)
        hits, sums = [], []
        for e in range(ROW_EXPERTS):
            hit = ids == first + e
            hits.append(jnp.sum(jnp.where(hit, 1.0, 0.0), axis=0, keepdims=True))
            sums.append(jnp.sum(jnp.where(hit, weights, 0.0), axis=0, keepdims=True))
        place = places(jnp.concatenate(hits, axis=0))
        for e in range(ROW_EXPERTS):
            wt[i, pl.ds(CAP * e, CAP), :] = jnp.where(slot == place[e : e + 1], sums[e], 0.0).astype(BF)

    def at(buf, i, w, t):
        return buf.at[i, :, :, pl.ds(pl.multiple_of(t * w, w), w)]

    def half(buf, i, w, t, e):
        return buf.at[i, e, :, pl.ds(pl.multiple_of(t * w, w), w)]

    def tp_send(buf, i, w, s, r, b):
        own = at(buf, i, w, tp)
        copy(own, own, s, r.at[0], fs, yp).start()
        copy(own, own, s, r.at[1], fs, ym).start()
        copy(own, own, s, b, fs, sib).start()

    def tp_pass(buf, i, w, s, r, b):
        a = at(buf, i, w, ym)
        arrived(a, r.at[0])
        h = half(buf, i, w, ym, 0)
        copy(h, h, s, r.at[2], fs, yp).start()
        copy(a, a, s, b, fs, sib).start()
        a = at(buf, i, w, yp)
        arrived(a, r.at[1])
        h = half(buf, i, w, yp, 1)
        copy(h, h, s, r.at[3], fs, ym).start()
        copy(a, a, s, b, fs, sib).start()

    def tp_last(buf, i, w, s, r, b):
        far = tpn(2, 0)
        for e in range(2):
            h = half(buf, i, w, far, e)
            arrived(h, r.at[2 + e])
            copy(h, h, s, b, fs, sib).start()

    def tp_done(buf, i, w, b):
        arrived(buf.at[i, :, :, pl.ds(0, 4 * w)], b)

    zs = (1, -1, 2, -2, 3, -3, 4, 0)
    peers = [(zs[(a + 2 * b) % NZ], (0, 1, 3, 2)[b]) for a in range(NZ) for b in range(NX)]
    peers = [p for p in peers if p != (0, 0)]
    gu_rows = pl.ds(pl.multiple_of(fs * KR, KR), KR)
    dn_rows = pl.ds(pl.multiple_of(fs * KD, KD), KD)

    def send_gu(n):
        f = fsn(*peers[n])
        copy(wgu.at[f], gu.at[:, gu_rows, :], ss.at[3], er.at[0], f, tp).start()

    def send_dn(n):
        f = fsn(*peers[n])
        copy(wdn.at[f], dn.at[:, dn_rows, :], ss.at[4], er.at[1], f, tp).start()

    def round_weights():
        for load in loads:
            load.wait()

        @pl.loop(0, NF)
        def _(f):
            for e in range(PER):
                wgu[f, e, :, :HC] = (fg[PER * f + e] * gain).astype(BF)
                wgu[f, e, :, HC:] = (fu[PER * f + e] * gain).astype(BF)
                wdn[f, e] = fd[PER * f + e].astype(BF)

        gu[:, gu_rows, :] = wgu[fs]
        dn[:, dn_rows, :] = wdn[fs]

    def gate_up(i):
        for e in range(PER):
            both = jnp.dot(xg[i, e], gu[e], preferred_element_type=F32)
            hg[i, e, :, hcols] = silu_mul(both[:, :HC], both[:, HC:]).astype(BF)

    def shared_gate_up():
        both = jnp.dot(nfull[...], tb[:, pl.ds(0, KR), :].reshape(D, 2 * HC), preferred_element_type=F32)
        mid = silu_mul(both[:, :HC], both[:, HC:]).astype(BF)
        hs[0, 0, :, hcols] = mid[: TOK // 2]
        hs[0, 1, :, hcols] = mid[TOK // 2 :]

    def down(i):
        for e in range(PER):
            out = jnp.dot(hg[i, e], dn[e], preferred_element_type=F32).astype(BF)
            for k in range(NX):
                og[i, k, pl.ds(CAP * e, CAP), :] = out[CAP * k : CAP * (k + 1)]

    def give_x(i):
        r1[i, x] = og[i, x]
        for dx in (1, 3, 2):
            k = lax.rem(x + dx, NX)
            copy(og.at[i, k], r1.at[i, x], ss.at[5], d1.at[i], fsn(0, dx), tp).start()

    def give_z(i):
        arrived(r1.at[i, pl.ds(0, NX - 1)], d1.at[i])
        part = lax.dot_general(
            wt[i], r1[i].reshape(NX * PER * CAP, DC), (((0,), (0,)), ((), ())), preferred_element_type=F32
        )
        d = OFFS[i]
        if d == 0:
            po[...] = part
            return
        far, base = (4, 0) if d > 0 else (3, 4)
        k = base + abs(d)
        if abs(d) < far:
            arrived(pr.at[k], dr.at[k])
            part = part + pr[k].astype(F32)
        pt[i] = part.astype(BF)
        copy(pt.at[i], pr.at[k - 1], ss.at[7], dr.at[k - 1], zp if d > 0 else zm, tp).start()

    tok = lambda i: (ta, i, ss.at[0], zr, xr)
    shr = lambda i: (tb, i, ss.at[8], szr, sxr)
    bq = lambda i: (xg, i, DC, ss.at[1], br.at[i], bs.at[i])
    cq = lambda i: (hg, i, HC, ss.at[2], cr.at[i], cs.at[i])
    shared = (hs, 0, HC, ss.at[6], cr.at[NZ], cs.at[NZ])

    def shared_gather(n):
        if 0 <= n < NZ:
            z_step(*shr(n))
        if 0 <= n - 1 < NZ:
            x_step(*shr(n - 1))
        if 0 <= n - 2 < NZ:
            x_last(*shr(n - 2))

    todo = [(send_gu, n) for n in range(NF - 1)] + [(send_dn, n) for n in range(NF - 1)]

    def flush(keep):
        while len(todo) > keep:
            send, n = todo.pop(0)
            send(n)

    def feed(k):
        if tick > 0:
            flush(len(todo) - min(FEED[k] if len(todo) >= NF else 2 * FEED[k], len(todo)))

    for tick in range(SECOND + NZ + LAG + 2):
        if tick < NZ:
            z_step(*tok(tick))
        if tick == 0:
            round_weights()
        feed(0)
        if 0 <= tick - 1 < NZ:
            x_step(*tok(tick - 1))
        feed(1)
        if 0 <= tick - 2 < NZ:
            x_last(*tok(tick - 2))
            select(tick - 2)
            tp_send(*bq(tick - 2))
        feed(2)
        if 0 <= tick - 3 < NZ:
            tp_pass(*bq(tick - 3))
        feed(3)
        if 0 <= tick - 4 < NZ:
            tp_last(*bq(tick - 4))
        feed(4)
        shared_gather(tick - SHARED)
        if tick < NZ:
            weigh(tick)
        t = tick - SECOND
        if t == 0:
            flush(NF - 1)
            arrived(gu.at[:, pl.ds(0, D - KR), :], er.at[0])
        if 0 <= t < NZ:
            i = ORDER[t]
            tp_done(xg, i, DC, bs.at[i])
            gate_up(i)
            tp_send(*cq(i))
        if 0 <= t - 1 < NZ:
            tp_pass(*cq(ORDER[t - 1]))
        if 0 <= t - 2 < NZ:
            tp_last(*cq(ORDER[t - 2]))
        n = tick - SHARED - NZ
        if n == 2:
            shared_gate_up()
            tp_send(*shared)
        elif n == 3:
            tp_pass(*shared)
        elif n == 4:
            tp_last(*shared)
        if 0 <= t - LAG < NZ:
            i = ORDER[t - LAG]
            if t == LAG:
                flush(0)
                arrived(dn.at[:, pl.ds(0, DE - KD), :], er.at[1])
            tp_done(hg, i, HC, cs.at[i])
            down(i)
            give_x(i)
        if 0 <= t - LAG - 1 < NZ:
            give_z(ORDER[t - LAG - 1])
        if t == NZ + 1:
            tp_done(hs, 0, HC, cs.at[NZ])
            sdn = tb[:, pl.ds(KR, KD), :].reshape(DE, DC)
            for e in range(2):
                sh[pl.ds(e * (TOK // 2), TOK // 2), :] = jnp.dot(hs[0, e], sdn, preferred_element_type=F32)
    total = sh[...] + po[...]
    for k in (4, 0):
        arrived(pr.at[k], dr.at[k])
        total = total + pr[k].astype(F32)
    mv[...] = total.astype(BF)

    def sent(ref, s):
        copy(ref, ref, s, dr.at[0], fs, sib).wait_send()

    sent(ta.at[pl.ds(0, NF - 1)], ss.at[0])
    sent(tb.at[pl.ds(0, NF - 1)], ss.at[8])
    sent(xg.at[pl.ds(0, NZ - 1)], ss.at[1])
    sent(hg.at[pl.ds(0, NZ - 1)], ss.at[2])
    sent(gu.at[:, pl.ds(0, D - KR), :], ss.at[3])
    sent(dn.at[:, pl.ds(0, DE - KD), :], ss.at[4])
    sent(r1.at[:, pl.ds(0, NX - 1)], ss.at[5])
    sent(hs.at[0, :, :, pl.ds(0, 7 * HC)], ss.at[6])
    sent(pr.at[pl.ds(0, NZ - 1)], ss.at[7])


def exchange(tokens, ids, rw, gain, sgate, sup, sdown, gate, up, down_w):
    vmem, anyw = pl.BlockSpec(memory_space=pltpu.VMEM), pl.BlockSpec(memory_space=pl.ANY)
    dma = pltpu.SemaphoreType.DMA
    return pl.pallas_call(
        kernel,
        out_shape=(
            pltpu.VMEM((PER, D, 2 * HC), BF),
            pltpu.VMEM((PER, DE, DC), BF),
            pltpu.VMEM((NF, KR + KD, DC), BF),
            pltpu.VMEM((TOK, DC), BF),
        ),
        in_specs=[anyw] * 10,
        out_specs=(vmem,) * 4,
        scratch_shapes=[
            pltpu.VMEM((TOK, D), BF),
            pltpu.VMEM((TOP_K, TOK), jnp.int32),
            pltpu.VMEM((TOP_K, TOK), F32),
            pltpu.VMEM((1, KR), F32),
            pltpu.VMEM((KR, HC), F32),
            pltpu.VMEM((KR, HC), F32),
            pltpu.VMEM((KD, DC), F32),
            pltpu.VMEM((EXPERTS, KR, HC), F32),
            pltpu.VMEM((EXPERTS, KR, HC), F32),
            pltpu.VMEM((EXPERTS, KD, DC), F32),
            pltpu.VMEM((NF, PER, KR, 2 * HC), BF),
            pltpu.VMEM((NF, PER, KD, DC), BF),
            pltpu.VMEM((TOK, D), BF),
            pltpu.VMEM((NF, TOK + 16, DC), BF),
            pltpu.VMEM((NZ, PER, SRC, D), BF),
            pltpu.VMEM((NZ, PER, SRC, DE), BF),
            pltpu.VMEM((1, 2, TOK // 2, DE), BF),
            pltpu.VMEM((NZ, NX, PER * CAP, DC), BF),
            pltpu.VMEM((NZ, ROW_EXPERTS * CAP, TOK), BF),
            pltpu.VMEM((NZ, NX, PER * CAP, DC), BF),
            pltpu.VMEM((NZ, TOK, DC), BF),
            pltpu.VMEM((NZ - 1, TOK, DC), BF),
            pltpu.VMEM((TOK, DC), F32),
            pltpu.VMEM((TOK, DC), F32),
            dma((9,)), dma((NZ, 4)), dma((9,)), dma((NZ, 4)), dma((NZ, 4)), dma((NZ,)), dma((NZ + 1, 4)),
            dma((NZ + 1,)), dma((2,)), dma((NZ,)), dma((NZ - 1,)), dma((9,)), dma((10,)),
        ],
        compiler_params=pltpu.CompilerParams(
            collective_id=0, has_side_effects=True, vmem_limit_bytes=54 * 1024 * 1024
        ),
    )(tokens, ids, rw, gain, sgate, sup, sdown, gate, up, down_w)


def writer(gu, dn, tb, mv, gate_o, up_o, dn_o, sg_o, su_o, sd_o, mixed_o, sems):
    left, right = pl.ds(0, HC), pl.ds(HC, HC)
    pairs = (
        (gu.at[:, :, left], gate_o),
        (gu.at[:, :, right], up_o),
        (dn, dn_o),
        (tb.at[:, pl.ds(0, KR), left], sg_o),
        (tb.at[:, pl.ds(0, KR), right], su_o),
        (tb.at[:, pl.ds(KR, KD), :], sd_o),
        (mv, mixed_o),
    )
    copies = [pltpu.make_async_copy(a, b, sems.at[k]) for k, (a, b) in enumerate(pairs)]
    for one in copies:
        one.start()
    for one in copies:
        one.wait()


def write_out(*arrays):
    shapes = ((PER, D, HC), (PER, D, HC), (PER, DE, DC), (NF, KR, HC), (NF, KR, HC), (NF, KD, DC), (TOK, DC))
    return pl.pallas_call(
        writer,
        out_shape=tuple(jax.ShapeDtypeStruct(s, BF) for s in shapes),
        in_specs=[pl.BlockSpec(memory_space=pltpu.VMEM)] * len(arrays),
        out_specs=(pl.BlockSpec(memory_space=pl.ANY),) * len(shapes),
        scratch_shapes=[pltpu.SemaphoreType.DMA((len(shapes),))],
        compiler_params=pltpu.CompilerParams(vmem_limit_bytes=8 * 1024 * 1024),
    )(*arrays)


def body(
    tokens,
    norm_gain,
    expert_gate,
    expert_up,
    expert_down,
    shared_gate,
    shared_up,
    shared_down,
    expert_ids,
    route_weights,
):
    results = exchange(
        tokens, expert_ids.T, route_weights.T, norm_gain[None], shared_gate, shared_up, shared_down,
        expert_gate, expert_up, expert_down,
    )
    gate_ready, up_ready, down_ready, sg, su, sd, mixed = write_out(*results)
    return (
        gate_ready,
        up_ready,
        down_ready,
        sg.reshape(D, HC),
        su.reshape(D, HC),
        sd.reshape(DE, DC),
        mixed,
    )


def solution(mesh):
    in_specs = (
        P("fs", None),
        P("fs"),
        P(None, "fs", "tp"),
        P(None, "fs", "tp"),
        P(None, "fs", "tp"),
        P("fs", "tp"),
        P("fs", "tp"),
        P("fs", "tp"),
        P("fs", None),
        P("fs", None),
    )
    out_specs = (
        P("fs", None, "tp"),
        P("fs", None, "tp"),
        P("fs", None, "tp"),
        P(None, "tp"),
        P(None, "tp"),
        P(None, "tp"),
        P("fs", "tp"),
    )
    return jax.shard_map(body, mesh=mesh, in_specs=in_specs, out_specs=out_specs, check_vma=False)
```
